32 devices in a mesh: ep: 8 (over z, y), tp: 4 (over x, core).
Axes of the slice: x: 2, y: 2, z: 4, core: 2. Of those that a mesh axis runs over, the one named last changes fastest.
Arguments:
- tokens_a: bfloat16 [1024, 2048], P('ep'), may hold values from -30 to 30
- attn_gain: float32 [2048], replicated, may hold values from 0.1 to 1.9
- w_query: bfloat16 [2048, 2048], P(None, 'tp'), may hold values from -2 to 2
- w_query_rot: bfloat16 [2048, 1024], P(None, 'tp'), may hold values from -0.125 to 0.125
- w_latent: bfloat16 [2048, 512], replicated, may hold values from -2 to 2
- w_key_rot: bfloat16 [2048, 32], replicated, may hold values from -0.125 to 0.125
- latent_gain: float32 [512], replicated, may hold values from 0.1 to 1.9
- w_key_up: bfloat16 [512, 2048], P(None, 'tp'), may hold values from -2 to 2
- w_value_up: bfloat16 [512, 2048], P(None, 'tp'), may hold values from -0.25 to 0.25
- w_output: bfloat16 [2048, 2048], P('tp'), may hold values from -0.125 to 0.125
- tokens_b: bfloat16 [2048, 2048], P('ep'), may hold values from -6 to 6
- ffn_gain: float32 [2048], replicated, may hold values from 0.1 to 1.9
- expert_ids: int32 [2048, 2], P('ep'), may hold values from 0 to 7, all different within a row; in each aligned block of 256 rows (0 to 255, 256 to 511, ...) at most 128 rows name the same one
- expert_weights: float32 [2048, 2], P('ep'), may hold values from 0.1 to 1
- w_gate: bfloat16 [8, 2048, 1024], P('ep', None, 'tp'), may hold values from -0.125 to 0.125
- w_up: bfloat16 [8, 2048, 1024], P('ep', None, 'tp'), may hold values from -0.125 to 0.125
- w_down: bfloat16 [8, 1024, 2048], P('ep', 'tp'), may hold values from -0.1875 to 0.1875
Outputs:
- mixed_a: bfloat16 [1024, 2048], P(('ep', 'tp'))
- mixed_b: bfloat16 [2048, 2048], P('ep', 'tp')
The draws below stay inside these ranges and needn't reach their ends.
Inputs may be any that keep to these rules, and one draw needn't show every extreme that they name: `expert_ids`: each row names 2 different experts. In the 256 rows of one index of ep no expert is named more than 128 times, and in some such block one expert is named exactly 128 times.
All inputs are finite; a program needn't handle non-finite values.
Results may differ from the reference program's by a relative error of at most 0.012.
Values may be sent and summed in bfloat16 or wider, within the bound.
A program may use at most 192 MiB of HBM per device.

```python
import math
import jax
import jax.numpy as jnp
import numpy as np
from jax import lax

D = 2048
HEADS = 32
NOPE = 64
ROPE = 32
VD = 64
KVR = 512
FFE = 1024
TOP_K = 2
ROWS_A = 128
ROWS_B = 256
EXPERTS = 8
SEQ_A = 1024
TOKENS_B = 2048
CAP = 128
N_EP = 8
N_TP = 4


def draw_tokens_a(key, part):
    entries = jnp.clip(jax.random.normal(jax.random.fold_in(key, 11), (SEQ_A, D), jnp.float32), -6.0, 6.0)
    return entries.astype(jnp.bfloat16)


def draw_w_query(key, part):
    drawn = jnp.clip(jax.random.normal(jax.random.fold_in(key, 21), (D, HEADS * NOPE), jnp.float32), -6.0, 6.0)
    drawn = drawn * D ** (-0.5)
    return jnp.clip(drawn, -2.0, 2.0).astype(jnp.bfloat16)


def draw_w_latent(key, part):
    drawn = jnp.clip(jax.random.normal(jax.random.fold_in(key, 31), (D, KVR), jnp.float32), -6.0, 6.0)
    drawn = drawn * D ** (-0.5)
    return jnp.clip(drawn, -2.0, 2.0).astype(jnp.bfloat16)


def draw_w_key_up(key, part):
    drawn = jnp.clip(jax.random.normal(jax.random.fold_in(key, 41), (KVR, HEADS * NOPE), jnp.float32), -6.0, 6.0)
    drawn = drawn * KVR ** (-0.5)
    return jnp.clip(drawn, -2.0, 2.0).astype(jnp.bfloat16)


def block_levels(own_key, extent, cuts, low, high):
    level = 1.0
    for dim, parts in cuts:
        draws = jax.random.uniform(jax.random.fold_in(jax.random.fold_in(own_key, 6), dim), (parts,), jnp.float32, low / len(cuts), high / len(cuts))
        level = level * jnp.repeat(jnp.exp(draws), extent[dim] // parts).reshape((-1,) + (1,) * (len(extent) - 1 - dim))
    return level


def deal_out(rng, own, number, rows, amount, top, limit, skew):
    sequence = jax.random.permutation(rng, amount)
    heavy_load, usual = portions_of(amount, rows * top, limit, skew, True), portions_of(amount, rows * top, limit, skew, False)
    places = jnp.arange(amount)

    def named(tallies, turn):
        used = int((tallies > 0).sum())
        fixed = max(1, used // 4)
        moved = fixed + (places - fixed + turn * (used - fixed)) % max(1, amount - fixed)
        return jnp.zeros((amount,), jnp.int32).at[sequence[jnp.where(places < fixed, places, moved)]].set(jnp.asarray(tallies, jnp.int32))

    tallies = jnp.where(number % 4 == 0, named(heavy_load, number // 4), named(usual, number - number // 4 - 1))
    mixed = jax.random.permutation(jax.random.fold_in(own, 3), amount)
    giver, taker = mixed[0:amount // 2 * 2:2], mixed[1:amount // 2 * 2:2]
    room = jnp.minimum(tallies[giver] - 1, limit - tallies[taker]) // 2
    room = jnp.where((giver == sequence[0]) | (taker == sequence[0]) | (tallies[taker] == 0), 0, jnp.maximum(room, 0))
    moved = jax.random.randint(jax.random.fold_in(own, 4), (amount // 2,), 0, 1 << 20) % (room + 1)
    tallies = tallies.at[giver].add(-moved).at[taker].add(moved)
    labels = jnp.searchsorted(jnp.cumsum(tallies), jnp.arange(rows * top), side="right").astype(jnp.int32)
    grid = labels.reshape(top, rows).T
    grid = grid[jax.random.permutation(jax.random.fold_in(own, 1), rows)]
    turn = jax.random.randint(jax.random.fold_in(own, 2), (rows, 1), 0, top)
    return jnp.take_along_axis(grid, (jnp.arange(top)[None, :] + turn) % top, axis=1)


def portions_of(amount, total, most, lean, full):
    weights = [(1 << 20) // math.isqrt(grade ** lean) + 1 for grade in range(1, amount + 1)]
    largest = most if full else min(most, max(-(-total // amount), total * weights[0] // sum(weights)))
    least = 1 if total - largest >= amount - 1 else 0
    given, surplus = [largest] + [least] * (amount - 1), total - largest - least * (amount - 1)
    while surplus > 0:
        movable = [i for i in range(1, amount) if given[i] < largest] or [i for i in range(1, amount) if given[i] < most]
        pool, left = sum([weights[i] for i in movable]), surplus
        for i in movable:
            more = min(most - given[i], max(1, left * weights[i] // pool), surplus)
            given[i] = given[i] + more
            surplus = surplus - more
    return np.array(given)


def scatter_about(key, dims, scale, reach, cuts=(), kind=jnp.bfloat16):
    level = block_levels(key, dims, cuts, -0.22, 0.18) if cuts else 1.0
    values = jax.random.normal(key, dims, jnp.float32) * scale * level
    return jnp.minimum(jnp.maximum(values, -reach), reach).astype(kind)


def setup_inputs(seed: int = 0) -> dict:
    seeds = jax.random.split(jax.random.key(seed), 18)
    tokens_a = draw_tokens_a(jax.random.fold_in(seeds[17], 71), 0)
    attn_gain = jnp.clip(1.0 + 0.18 * jax.random.normal(seeds[1], (D,), jnp.float32), 0.1, 1.9)
    w_query = draw_w_query(jax.random.fold_in(seeds[17], 71), 0)
    w_query_rot = scatter_about(seeds[3], (D, HEADS * ROPE), D ** -0.5, 0.125, ((1, 4),))
    w_latent = draw_w_latent(jax.random.fold_in(seeds[17], 71), 0)
    w_key_rot = scatter_about(seeds[5], (D, ROPE), D ** -0.5, 0.125)
    latent_gain = jnp.clip(1.0 + 0.18 * jax.random.normal(seeds[6], (KVR,), jnp.float32), 0.1, 1.9)
    w_key_up = draw_w_key_up(jax.random.fold_in(seeds[17], 71), 0)
    w_value_up = scatter_about(seeds[8], (KVR, HEADS * VD), KVR ** -0.5, 0.25, ((1, 4),))
    w_output = scatter_about(seeds[9], (HEADS * VD, D), (HEADS * VD) ** -0.5, 0.125, ((0, 4),))
    tokens_b = scatter_about(seeds[10], (TOKENS_B, D), 1.0, 6.0, ((0, 8),))
    ffn_gain = jnp.clip(1.0 + 0.18 * jax.random.normal(seeds[11], (D,), jnp.float32), 0.1, 1.9)
    expert_ids_keys = jax.random.split(jax.random.fold_in(seeds[12], 1), TOKENS_B // ROWS_B)
    expert_ids_turns = jax.random.permutation(jax.random.fold_in(seeds[12], 3), TOKENS_B // ROWS_B)
    expert_ids = jax.vmap(lambda own, number: deal_out(jax.random.fold_in(seeds[12], 2), own, number, ROWS_B, EXPERTS, TOP_K, CAP, 1))(expert_ids_keys, expert_ids_turns).reshape((TOKENS_B, TOP_K))
    expert_weights = jnp.clip(0.1 + 0.9 * jax.random.uniform(seeds[13], (TOKENS_B, TOP_K), jnp.float32) ** block_levels(seeds[13], (TOKENS_B, TOP_K), ((0, 8),), -0.2, 0.2), 0.1, 1.0)
    w_gate = scatter_about(seeds[14], (EXPERTS, D, FFE), D ** -0.5, 0.125, ((0, 8), (2, 4)))
    w_up = scatter_about(seeds[15], (EXPERTS, D, FFE), D ** -0.5, 0.125, ((0, 8), (2, 4)))
    w_down = scatter_about(seeds[16], (EXPERTS, FFE, D), FFE ** -0.5, 0.1875, ((0, 8), (1, 4)))
    return dict(tokens_a=tokens_a, attn_gain=attn_gain, w_query=w_query, w_query_rot=w_query_rot, w_latent=w_latent, w_key_rot=w_key_rot, latent_gain=latent_gain, w_key_up=w_key_up, w_value_up=w_value_up, w_output=w_output, tokens_b=tokens_b, ffn_gain=ffn_gain, expert_ids=expert_ids, expert_weights=expert_weights, w_gate=w_gate, w_up=w_up, w_down=w_down)


epsilon = 1e-06
rope_base = 10000.0

def normalize(matrix, gain):
    floats = matrix.astype(jnp.float32)
    scaled = floats * lax.rsqrt(lax.optimization_barrier(jnp.mean(floats * floats, axis=-1, keepdims=True)) + epsilon)
    return scaled * gain.astype(jnp.float32)

def rotate(vectors, positions):
    rot_width = vectors.shape[-1]
    half_width = rot_width // 2
    inverse = rope_base ** (-(jnp.arange(half_width, dtype=jnp.float32) * 2.0) / rot_width)
    angles = positions.astype(jnp.float32)[:, None] * inverse[None, :]
    cosine = jnp.cos(angles)[:, None, :]
    sine_part = jnp.sin(angles)[:, None, :]
    first_half = vectors[..., :half_width]
    second_half = vectors[..., half_width:]
    return jnp.concatenate([first_half * cosine - second_half * sine_part, first_half * sine_part + second_half * cosine], axis=-1)

def attention_half(tokens_a, attn_gain, w_query, w_query_rot, w_latent, w_key_rot, latent_gain, w_key_up, w_value_up, w_output):
    positions = jnp.arange(SEQ_A, dtype=jnp.int32)
    normed = normalize(tokens_a, attn_gain).astype(jnp.bfloat16)
    query_plain = jnp.dot(normed, w_query, preferred_element_type=jnp.float32).astype(jnp.bfloat16)
    query_plain = query_plain.reshape(N_EP, ROWS_A, HEADS, NOPE)
    turned = jnp.dot(normed, w_query_rot, preferred_element_type=jnp.float32).reshape(SEQ_A, HEADS, ROPE)
    query_rotated_rows = rotate(turned, positions).astype(jnp.bfloat16).reshape(N_EP, ROWS_A, HEADS, ROPE)
    latent = normalize(jnp.dot(normed, w_latent, preferred_element_type=jnp.float32), latent_gain).astype(jnp.bfloat16)
    key_raw = jnp.dot(normed, w_key_rot, preferred_element_type=jnp.float32)[:, None, :]
    key_turned = rotate(key_raw, positions)[:, 0, :].astype(jnp.bfloat16)
    key_plain = jnp.dot(latent, w_key_up, preferred_element_type=jnp.float32).astype(jnp.bfloat16)
    values = jnp.dot(latent, w_value_up, preferred_element_type=jnp.float32).astype(jnp.bfloat16)
    key_wide_float = key_plain.astype(jnp.float32).reshape(N_EP, ROWS_A, HEADS, NOPE)
    rotated_key_float = key_turned.astype(jnp.float32).reshape(N_EP, ROWS_A, ROPE)
    value_float = values.astype(jnp.float32).reshape(N_EP, ROWS_A, HEADS, VD)
    key_pos = positions.reshape(N_EP, ROWS_A)
    logit_scale = (NOPE + ROPE) ** (-0.5)

    def one_block(inputs):
        query_tile_block, rotated_key_block, query_pos = inputs
        score_matrix = (jnp.einsum('yvz,wrvz->yvwr', query_tile_block.astype(jnp.float32), key_wide_float) + jnp.einsum('yjx,inx->yjin', rotated_key_block.astype(jnp.float32), rotated_key_float)) * logit_scale
        allowed = key_pos[None, None, :, :] <= query_pos[:, None, None, None]
        masked = jnp.where(allowed, score_matrix, -1e+30)
        block_max = lax.optimization_barrier(jnp.max(masked, axis=-1))
        probs = jnp.where(allowed, jnp.exp(masked - block_max[..., None]), 0.0)
        block_total = lax.optimization_barrier(jnp.sum(probs, axis=-1))
        rounded = probs.astype(jnp.bfloat16).astype(jnp.float32)
        block_out = jnp.einsum('qhbk,bkhd->qhbd', rounded, value_float)
        overall = lax.optimization_barrier(jnp.max(block_max, axis=-1))
        factor = jnp.exp(block_max - overall[..., None])
        denominator = lax.optimization_barrier(jnp.sum(factor * block_total, axis=-1))
        merged = lax.optimization_barrier(jnp.sum(factor[..., None] * block_out, axis=2))
        return (merged / denominator[..., None]).astype(jnp.bfloat16).reshape(ROWS_A, HEADS * VD)
    attended = lax.map(one_block, (query_plain, query_rotated_rows, key_pos)).reshape(SEQ_A, HEADS * VD)
    group_width = HEADS // N_TP * VD
    summed = jnp.zeros((SEQ_A, D), jnp.float32)
    for lane_index in range(N_TP):
        lane_part = jnp.dot(attended[:, lane_index * group_width:(lane_index + 1) * group_width], w_output[lane_index * group_width:(lane_index + 1) * group_width], preferred_element_type=jnp.float32)
        summed = summed + lax.optimization_barrier(lane_part.astype(jnp.bfloat16)).astype(jnp.float32)
    return summed.astype(jnp.bfloat16)

def expert_half(tokens_b, ffn_gain, expert_ids, expert_weights, w_gate, w_up, w_down):
    normed = normalize(tokens_b, ffn_gain).astype(jnp.bfloat16)
    block_pairs = ROWS_B * TOP_K
    flat_ids = expert_ids.reshape(N_EP, block_pairs)
    onehot = (flat_ids[:, :, None] == jnp.arange(EXPERTS, dtype=jnp.int32)[None, None, :]).astype(jnp.int32)
    before = jnp.cumsum(onehot, axis=1) - onehot
    slot_index = lax.optimization_barrier(jnp.sum(before * onehot, axis=2))
    block_index = jnp.arange(N_EP, dtype=jnp.int32)[:, None]
    target = (flat_ids * (N_EP * CAP) + block_index * CAP + slot_index).reshape(-1).astype(jnp.int32)
    total_slots = EXPERTS * N_EP * CAP
    pair_total = TOKENS_B * TOP_K
    source_row = jnp.zeros((total_slots,), jnp.int32).at[target].set(jnp.arange(pair_total, dtype=jnp.int32) // TOP_K)
    occupied = jnp.zeros((total_slots,), jnp.int32).at[target].set(1)
    table = source_row.reshape(EXPERTS, N_EP * CAP)
    filled = occupied.reshape(EXPERTS, N_EP * CAP)
    lane_width = FFE // N_TP

    def one_expert(inputs):
        rows_of, filled_of, gate_weight, up_weight, down_weight = inputs
        taken_rows = jnp.where(filled_of[:, None] > 0, normed[rows_of], jnp.zeros((), jnp.bfloat16))
        gate_part = jnp.dot(taken_rows, gate_weight, preferred_element_type=jnp.float32)
        up_part = jnp.dot(taken_rows, up_weight, preferred_element_type=jnp.float32)
        hidden = (jax.nn.silu(gate_part) * up_part).astype(jnp.bfloat16)
        summed = jnp.zeros((taken_rows.shape[0], D), jnp.float32)
        for lane_index in range(N_TP):
            lane_part = jnp.dot(hidden[:, lane_index * lane_width:(lane_index + 1) * lane_width], down_weight[lane_index * lane_width:(lane_index + 1) * lane_width], preferred_element_type=jnp.float32)
            summed = summed + lax.optimization_barrier(lane_part.astype(jnp.bfloat16)).astype(jnp.float32)
        return summed.astype(jnp.bfloat16)
    outputs = lax.map(one_expert, (table, filled, w_gate, w_up, w_down))
    picked = outputs.reshape(total_slots, D)[target].astype(jnp.float32).reshape(TOKENS_B, TOP_K, D)
    shares = expert_weights / lax.optimization_barrier(jnp.sum(expert_weights, axis=1, keepdims=True))
    return lax.optimization_barrier(jnp.sum(picked * shares[:, :, None], axis=1)).astype(jnp.bfloat16)

def reference(tokens_a, attn_gain, w_query, w_query_rot, w_latent, w_key_rot, latent_gain, w_key_up, w_value_up, w_output, tokens_b, ffn_gain, expert_ids, expert_weights, w_gate, w_up, w_down):
    mixed_a = attention_half(tokens_a, attn_gain, w_query, w_query_rot, w_latent, w_key_rot, latent_gain, w_key_up, w_value_up, w_output)
    mixed_b = expert_half(tokens_b, ffn_gain, expert_ids, expert_weights, w_gate, w_up, w_down)
    return (mixed_a, mixed_b)
```

```python
import jax
import jax.numpy as jnp
from jax import lax
from jax.sharding import PartitionSpec as P

NOPE = 64
ROPE = 32
VD = 64


epsilon = 1e-06
rope_base = 10000.0


def normalize(matrix, gain):
    floats = matrix.astype(jnp.float32)
    scaled = floats * lax.rsqrt(jnp.mean(floats * floats, axis=-1, keepdims=True) + epsilon)
    return scaled * gain


def rotate(vectors, positions):
    rot_width = vectors.shape[-1]
    half_width = rot_width // 2
    inverse = rope_base ** (-(jnp.arange(half_width, dtype=jnp.float32) * 2.0) / rot_width)
    angles = positions.astype(jnp.float32)[:, None] * inverse[None, :]
    cosine = jnp.cos(angles)[:, None, :]
    sine_part = jnp.sin(angles)[:, None, :]
    first_half = vectors[..., :half_width]
    second_half = vectors[..., half_width:]
    return jnp.concatenate(
        [
            first_half * cosine - second_half * sine_part,
            first_half * sine_part + second_half * cosine,
        ],
        axis=-1,
    )


def attention_half(
    tokens_a,
    attn_gain,
    w_query,
    w_query_rot,
    w_latent,
    w_key_rot,
    latent_gain,
    w_key_up,
    w_value_up,
    w_output,
    outgoing,
):
    row_count = tokens_a.shape[0]
    head_count = w_query.shape[1] // NOPE
    offset = lax.axis_index("ep") * row_count
    positions = offset + jnp.arange(row_count, dtype=jnp.int32)
    normed = normalize(tokens_a, attn_gain).astype(jnp.bfloat16)
    query_plain = jnp.dot(normed, w_query, preferred_element_type=jnp.float32).astype(jnp.bfloat16)
    query_plain = query_plain.reshape(row_count, head_count, NOPE)
    turned = jnp.dot(normed, w_query_rot, preferred_element_type=jnp.float32).reshape(
        row_count, head_count, ROPE
    )
    query_rotated_rows = rotate(turned, positions).astype(jnp.bfloat16)
    latent = normalize(
        jnp.dot(normed, w_latent, preferred_element_type=jnp.float32), latent_gain
    ).astype(jnp.bfloat16)
    key_raw = jnp.dot(normed, w_key_rot, preferred_element_type=jnp.float32)[:, None, :]
    key_turned = rotate(key_raw, positions)[:, 0, :].astype(jnp.bfloat16)
    logit_scale = (NOPE + ROPE) ** (-0.5)
    outgoing, compact = lax.optimization_barrier(
        (outgoing, jnp.concatenate([latent, key_turned], axis=1))
    )
    joined = lax.all_gather(compact, "ep", axis=0, tiled=True)
    arrived = lax.all_to_all(outgoing, "ep", split_axis=0, concat_axis=0, tiled=True)
    joined, arrived = lax.optimization_barrier((joined, arrived))
    pieces = (joined[:, : latent.shape[1]], joined[:, latent.shape[1] :])
    piece_keys = jnp.dot(pieces[0], w_key_up, preferred_element_type=jnp.float32).astype(
        jnp.bfloat16
    )
    piece_values = jnp.dot(pieces[0], w_value_up, preferred_element_type=jnp.float32).astype(
        jnp.bfloat16
    )
    key_count = piece_keys.shape[0]
    blocks = key_count // row_count
    key_blocks = piece_keys.reshape(blocks, row_count, head_count, NOPE)
    value_blocks = piece_values.reshape(blocks, row_count, head_count, VD)
    rotated_key_blocks = pieces[1].reshape(blocks, row_count, ROPE)
    score_matrix = (
        jnp.einsum("yvz,wrvz->yvwr", query_plain, key_blocks, preferred_element_type=jnp.float32)
        + jnp.einsum(
            "yjx,inx->yjin",
            query_rotated_rows,
            rotated_key_blocks,
            preferred_element_type=jnp.float32,
        )
    ) * logit_scale
    key_pos = jnp.arange(key_count, dtype=jnp.int32).reshape(blocks, row_count)
    allowed = key_pos[None, None, :, :] <= positions[:, None, None, None]
    masked = jnp.where(allowed, score_matrix, -1e30)
    block_max = jnp.max(masked, axis=-1)
    probs = jnp.where(allowed, jnp.exp(masked - block_max[..., None]), 0.0)
    block_total = jnp.sum(probs, axis=-1)
    block_out = jnp.einsum(
        "qhbk,bkhd->qhbd",
        probs.astype(jnp.bfloat16),
        value_blocks,
        preferred_element_type=jnp.float32,
    )
    run_max = jnp.full((row_count, head_count), -1e30, jnp.float32)
    new_max = jnp.maximum(run_max, jnp.max(block_max, axis=-1))
    new_factor = jnp.exp(block_max - new_max[..., None])
    new_total = jnp.sum(new_factor * block_total, axis=-1)
    new_out = jnp.sum(new_factor[..., None] * block_out, axis=2)
    attended = (
        (new_out / new_total[..., None]).astype(jnp.bfloat16).reshape(row_count, head_count * VD)
    )
    mixed = lax.psum_scatter(
        jnp.dot(attended, w_output, preferred_element_type=jnp.float32).astype(jnp.bfloat16),
        "tp",
        scatter_dimension=0,
        tiled=True,
    )
    return mixed, arrived


def dispatch_rows(tokens_b, ffn_gain, expert_ids, expert_count):
    row_count, width = tokens_b.shape
    top_count = expert_ids.shape[1]
    capacity = 2 * row_count * top_count // expert_count
    tp_count = lax.axis_size("tp")
    part_width = width // tp_count
    floats = tokens_b.astype(jnp.float32)
    factor = lax.rsqrt(jnp.mean(floats * floats, axis=-1, keepdims=True) + epsilon)
    start = lax.axis_index("tp") * part_width
    own = lax.dynamic_slice_in_dim(tokens_b, start, part_width, 1).astype(jnp.float32)
    own_gain = lax.dynamic_slice_in_dim(ffn_gain, start, part_width, 0)
    normed = (own * factor * own_gain).astype(jnp.bfloat16)
    experts = jnp.arange(expert_count, dtype=jnp.int32)
    slots = jnp.arange(capacity, dtype=jnp.int32)
    named = (expert_ids[:, :, None] == experts).any(axis=1)
    rows = jnp.arange(row_count, dtype=jnp.int32)
    earlier = (rows[:, None] > rows[None, :]).astype(jnp.bfloat16)
    before = jnp.dot(
        earlier, named.astype(jnp.bfloat16), preferred_element_type=jnp.float32
    ).astype(jnp.int32)
    slot_of = jnp.where(named, before, -1).T
    chosen = (slot_of[:, None, :] == slots[None, :, None]).astype(jnp.bfloat16)
    outgoing = jnp.dot(
        chosen.reshape(expert_count * capacity, row_count),
        normed,
        preferred_element_type=jnp.float32,
    ).astype(jnp.bfloat16)
    outgoing = outgoing.reshape(expert_count, capacity, part_width)
    return outgoing, before


def swap(block, distance, count):
    return lax.ppermute(block, "tp", [(i, i ^ distance) for i in range(count)])


def expert_half(arrived, before, expert_ids, expert_weights, w_gate, w_up, w_down):
    expert_count, capacity, part_width = arrived.shape
    tp_count = lax.axis_size("tp")
    top_count = expert_ids.shape[1]
    experts = jnp.arange(expert_count, dtype=jnp.int32)
    me = lax.axis_index("tp")
    blocks = {0: arrived.reshape(-1, part_width)}
    distance = tp_count // 2
    while distance:
        for mask in list(blocks):
            blocks[mask ^ distance] = swap(blocks[mask], distance, tp_count)
        distance //= 2
    gate_part = 0.0
    up_part = 0.0
    for mask, block in blocks.items():
        first = (me ^ mask) * part_width
        gate_rows = lax.dynamic_slice_in_dim(w_gate[0], first, part_width, 0)
        up_rows = lax.dynamic_slice_in_dim(w_up[0], first, part_width, 0)
        gate_part += jnp.dot(block, gate_rows, preferred_element_type=jnp.float32)
        up_part += jnp.dot(block, up_rows, preferred_element_type=jnp.float32)
    hidden = (jax.nn.silu(gate_part) * up_part).astype(jnp.bfloat16)
    parts = {}
    for mask in reversed(range(tp_count)):
        down_columns = lax.dynamic_slice_in_dim(w_down[0], (me ^ mask) * part_width, part_width, 1)
        parts[mask] = jnp.dot(hidden, down_columns, preferred_element_type=jnp.float32)
    distance = 1
    while distance < tp_count:
        for mask in [m for m in parts if m & distance]:
            came = swap(parts.pop(mask).astype(jnp.bfloat16), distance, tp_count)
            parts[mask ^ distance] += came.astype(jnp.float32)
        distance *= 2
    summed = parts[0].astype(jnp.bfloat16)
    returned = lax.all_to_all(
        summed.reshape(expert_count, capacity, part_width),
        "ep",
        split_axis=0,
        concat_axis=0,
        tiled=True,
    )
    shares = expert_weights / jnp.sum(expert_weights, axis=1, keepdims=True)
    table = returned.reshape(expert_count * capacity, part_width)
    total = 0.0
    for k in range(top_count):
        own_slot = jnp.sum(jnp.where(expert_ids[:, k : k + 1] == experts, before, 0), axis=1)
        target = expert_ids[:, k] * capacity + own_slot
        pick = (
            target[:, None] == jnp.arange(expert_count * capacity, dtype=jnp.int32)
        ).astype(jnp.bfloat16)
        picked = jnp.dot(pick, table, preferred_element_type=jnp.float32)
        total = total + picked * shares[:, k : k + 1]
    return total.astype(jnp.bfloat16)


def on_device(
    tokens_a,
    attn_gain,
    w_query,
    w_query_rot,
    w_latent,
    w_key_rot,
    latent_gain,
    w_key_up,
    w_value_up,
    w_output,
    tokens_b,
    ffn_gain,
    expert_ids,
    expert_weights,
    w_gate,
    w_up,
    w_down,
):
    expert_count = w_gate.shape[0] * lax.axis_size("ep")
    outgoing, before = dispatch_rows(tokens_b, ffn_gain, expert_ids, expert_count)
    mixed_a, arrived = attention_half(
        tokens_a,
        attn_gain,
        w_query,
        w_query_rot,
        w_latent,
        w_key_rot,
        latent_gain,
        w_key_up,
        w_value_up,
        w_output,
        outgoing,
    )
    mixed_b = expert_half(arrived, before, expert_ids, expert_weights, w_gate, w_up, w_down)
    return (mixed_a, mixed_b)


def solution(mesh):
    placed = (
        P("ep", None),
        P(),
        P(None, "tp"),
        P(None, "tp"),
        P(),
        P(),
        P(),
        P(None, "tp"),
        P(None, "tp"),
        P("tp", None),
        P("ep", None),
        P(),
        P("ep", None),
        P("ep", None),
        P("ep", None, "tp"),
        P("ep", None, "tp"),
        P("ep", "tp", None),
    )
    return jax.shard_map(
        on_device,
        mesh=mesh,
        in_specs=placed,
        out_specs=(P(("ep", "tp"), None), P("ep", "tp")),
        check_vma=False,
    )
```

```python
import jax
import jax.numpy as jnp
from jax import lax
from jax.sharding import PartitionSpec as P

NOPE = 64
ROPE = 32
VD = 64


epsilon = 1e-06
rope_base = 10000.0


def normalize(matrix, gain):
    floats = matrix.astype(jnp.float32)
    scaled = floats * lax.rsqrt(jnp.mean(floats * floats, axis=-1, keepdims=True) + epsilon)
    return scaled * gain


def rotate(vectors, positions):
    rot_width = vectors.shape[-1]
    half_width = rot_width // 2
    inverse = rope_base ** (-(jnp.arange(half_width, dtype=jnp.float32) * 2.0) / rot_width)
    angles = positions.astype(jnp.float32)[:, None] * inverse[None, :]
    cosine = jnp.cos(angles)[:, None, :]
    sine_part = jnp.sin(angles)[:, None, :]
    first_half = vectors[..., :half_width]
    second_half = vectors[..., half_width:]
    return jnp.concatenate(
        [
            first_half * cosine - second_half * sine_part,
            first_half * sine_part + second_half * cosine,
        ],
        axis=-1,
    )


def attention_half(
    tokens_a,
    attn_gain,
    w_query,
    w_query_rot,
    w_latent,
    w_key_rot,
    latent_gain,
    w_key_up,
    w_value_up,
    w_output,
    outgoing,
):
    row_count = tokens_a.shape[0]
    head_count = w_query.shape[1] // NOPE
    offset = lax.axis_index("ep") * row_count
    positions = offset + jnp.arange(row_count, dtype=jnp.int32)
    normed = normalize(tokens_a, attn_gain).astype(jnp.bfloat16)
    query_plain = jnp.dot(normed, w_query, preferred_element_type=jnp.float32).astype(jnp.bfloat16)
    query_plain = query_plain.reshape(row_count, head_count, NOPE)
    turned = jnp.dot(normed, w_query_rot, preferred_element_type=jnp.float32).reshape(
        row_count, head_count, ROPE
    )
    query_rotated_rows = rotate(turned, positions).astype(jnp.bfloat16)
    latent = normalize(
        jnp.dot(normed, w_latent, preferred_element_type=jnp.float32), latent_gain
    ).astype(jnp.bfloat16)
    key_raw = jnp.dot(normed, w_key_rot, preferred_element_type=jnp.float32)[:, None, :]
    key_turned = rotate(key_raw, positions)[:, 0, :].astype(jnp.bfloat16)
    logit_scale = (NOPE + ROPE) ** (-0.5)
    outgoing, compact = lax.optimization_barrier(
        (outgoing, jnp.concatenate([latent, key_turned], axis=1))
    )
    joined = lax.all_gather(compact, "ep", axis=0, tiled=True)
    arrived = lax.all_to_all(outgoing, "ep", split_axis=0, concat_axis=0, tiled=True)
    pieces = (joined[:, : latent.shape[1]], joined[:, latent.shape[1] :])
    piece_keys = jnp.dot(pieces[0], w_key_up, preferred_element_type=jnp.float32).astype(
        jnp.bfloat16
    )
    piece_values = jnp.dot(pieces[0], w_value_up, preferred_element_type=jnp.float32).astype(
        jnp.bfloat16
    )
    key_count = piece_keys.shape[0]
    blocks = key_count // row_count
    key_blocks = piece_keys.reshape(blocks, row_count, head_count, NOPE)
    value_blocks = piece_values.reshape(blocks, row_count, head_count, VD)
    rotated_key_blocks = pieces[1].reshape(blocks, row_count, ROPE)
    score_matrix = (
        jnp.einsum("yvz,wrvz->yvwr", query_plain, key_blocks, preferred_element_type=jnp.float32)
        + jnp.einsum(
            "yjx,inx->yjin",
            query_rotated_rows,
            rotated_key_blocks,
            preferred_element_type=jnp.float32,
        )
    ) * logit_scale
    key_pos = jnp.arange(key_count, dtype=jnp.int32).reshape(blocks, row_count)
    allowed = key_pos[None, None, :, :] <= positions[:, None, None, None]
    masked = jnp.where(allowed, score_matrix, -1e30)
    block_max = jnp.max(masked, axis=-1)
    probs = jnp.where(allowed, jnp.exp(masked - block_max[..., None]), 0.0)
    block_total = jnp.sum(probs, axis=-1)
    block_out = jnp.einsum(
        "qhbk,bkhd->qhbd",
        probs.astype(jnp.bfloat16),
        value_blocks,
        preferred_element_type=jnp.float32,
    )
    run_max = jnp.full((row_count, head_count), -1e30, jnp.float32)
    new_max = jnp.maximum(run_max, jnp.max(block_max, axis=-1))
    new_factor = jnp.exp(block_max - new_max[..., None])
    new_total = jnp.sum(new_factor * block_total, axis=-1)
    new_out = jnp.sum(new_factor[..., None] * block_out, axis=2)
    attended = (
        (new_out / new_total[..., None]).astype(jnp.bfloat16).reshape(row_count, head_count * VD)
    )
    mixed = lax.psum_scatter(
        jnp.dot(attended, w_output, preferred_element_type=jnp.float32).astype(jnp.bfloat16),
        "tp",
        scatter_dimension=0,
        tiled=True,
    )
    return mixed, arrived


def dispatch_rows(tokens_b, ffn_gain, expert_ids, expert_count):
    row_count, width = tokens_b.shape
    top_count = expert_ids.shape[1]
    capacity = 2 * row_count * top_count // expert_count
    tp_count = lax.axis_size("tp")
    part_width = width // tp_count
    floats = tokens_b.astype(jnp.float32)
    factor = lax.rsqrt(jnp.mean(floats * floats, axis=-1, keepdims=True) + epsilon)
    start = lax.axis_index("tp") * part_width
    own = lax.dynamic_slice_in_dim(tokens_b, start, part_width, 1).astype(jnp.float32)
    own_gain = lax.dynamic_slice_in_dim(ffn_gain, start, part_width, 0)
    normed = (own * factor * own_gain).astype(jnp.bfloat16)
    experts = jnp.arange(expert_count, dtype=jnp.int32)
    slots = jnp.arange(capacity, dtype=jnp.int32)
    named = (expert_ids[:, :, None] == experts).any(axis=1)
    rows = jnp.arange(row_count, dtype=jnp.int32)
    earlier = (rows[:, None] > rows[None, :]).astype(jnp.bfloat16)
    before = jnp.dot(
        earlier, named.astype(jnp.bfloat16), preferred_element_type=jnp.float32
    ).astype(jnp.int32)
    slot_of = jnp.where(named, before, -1).T
    chosen = (slot_of[:, None, :] == slots[None, :, None]).astype(jnp.bfloat16)
    outgoing = jnp.dot(
        chosen.reshape(expert_count * capacity, row_count),
        normed,
        preferred_element_type=jnp.float32,
    ).astype(jnp.bfloat16)
    outgoing = outgoing.reshape(expert_count, capacity, part_width)
    return outgoing, before


def swap(block, distance, count):
    return lax.ppermute(block, "tp", [(i, i ^ distance) for i in range(count)])


def expert_half(arrived, before, expert_ids, expert_weights, w_gate, w_up, w_down):
    expert_count, capacity, part_width = arrived.shape
    tp_count = lax.axis_size("tp")
    top_count = expert_ids.shape[1]
    experts = jnp.arange(expert_count, dtype=jnp.int32)
    me = lax.axis_index("tp")
    blocks = {0: arrived.reshape(-1, part_width)}
    distance = tp_count // 2
    while distance:
        for mask in list(blocks):
            blocks[mask ^ distance] = swap(blocks[mask], distance, tp_count)
        distance //= 2
    gate_part = 0.0
    up_part = 0.0
    for mask, block in blocks.items():
        first = (me ^ mask) * part_width
        gate_rows = lax.dynamic_slice_in_dim(w_gate[0], first, part_width, 0)
        up_rows = lax.dynamic_slice_in_dim(w_up[0], first, part_width, 0)
        gate_part += jnp.dot(block, gate_rows, preferred_element_type=jnp.float32)
        up_part += jnp.dot(block, up_rows, preferred_element_type=jnp.float32)
    hidden = (jax.nn.silu(gate_part) * up_part).astype(jnp.bfloat16)
    parts = {}
    for mask in reversed(range(tp_count)):
        down_columns = lax.dynamic_slice_in_dim(w_down[0], (me ^ mask) * part_width, part_width, 1)
        parts[mask] = jnp.dot(hidden, down_columns, preferred_element_type=jnp.float32)
    distance = 1
    while distance < tp_count:
        for mask in [m for m in parts if m & distance]:
            came = swap(parts.pop(mask).astype(jnp.bfloat16), distance, tp_count)
            parts[mask ^ distance] += came.astype(jnp.float32)
        distance *= 2
    summed = parts[0].astype(jnp.bfloat16)
    returned = lax.all_to_all(
        summed.reshape(expert_count, capacity, part_width),
        "ep",
        split_axis=0,
        concat_axis=0,
        tiled=True,
    )
    shares = expert_weights / jnp.sum(expert_weights, axis=1, keepdims=True)
    table = returned.reshape(expert_count * capacity, part_width)
    total = 0.0
    for k in range(top_count):
        own_slot = jnp.sum(jnp.where(expert_ids[:, k : k + 1] == experts, before, 0), axis=1)
        target = expert_ids[:, k] * capacity + own_slot
        pick = (
            target[:, None] == jnp.arange(expert_count * capacity, dtype=jnp.int32)
        ).astype(jnp.bfloat16)
        picked = jnp.dot(pick, table, preferred_element_type=jnp.float32)
        total = total + picked * shares[:, k : k + 1]
    return total.astype(jnp.bfloat16)


def on_device(
    tokens_a,
    attn_gain,
    w_query,
    w_query_rot,
    w_latent,
    w_key_rot,
    latent_gain,
    w_key_up,
    w_value_up,
    w_output,
    tokens_b,
    ffn_gain,
    expert_ids,
    expert_weights,
    w_gate,
    w_up,
    w_down,
):
    expert_count = w_gate.shape[0] * lax.axis_size("ep")
    outgoing, before = dispatch_rows(tokens_b, ffn_gain, expert_ids, expert_count)
    mixed_a, arrived = attention_half(
        tokens_a,
        attn_gain,
        w_query,
        w_query_rot,
        w_latent,
        w_key_rot,
        latent_gain,
        w_key_up,
        w_value_up,
        w_output,
        outgoing,
    )
    mixed_b = expert_half(arrived, before, expert_ids, expert_weights, w_gate, w_up, w_down)
    return (mixed_a, mixed_b)


def solution(mesh):
    placed = (
        P("ep", None),
        P(),
        P(None, "tp"),
        P(None, "tp"),
        P(),
        P(),
        P(),
        P(None, "tp"),
        P(None, "tp"),
        P("tp", None),
        P("ep", None),
        P(),
        P("ep", None),
        P("ep", None),
        P("ep", None, "tp"),
        P("ep", None, "tp"),
        P("ep", "tp", None),
    )
    return jax.shard_map(
        on_device,
        mesh=mesh,
        in_specs=placed,
        out_specs=(P(("ep", "tp"), None), P("ep", "tp")),
        check_vma=False,
    )
```
